256 devices in a mesh: grp: 4 (over y, x), ep: 32 (over z), tp: 2 (over core).
Axes of the slice: x: 2, y: 2, z: 32, core: 2. Of those that a mesh axis runs over, the one named last changes fastest.
The devices are a block of a 4x16x32 slice.
Arguments:
- tokens: bfloat16 [65536, 2048], P(('grp', 'ep', 'tp')), parts along dimension 0, may hold values from -6 to 6
- norm_gain: float32 [2048], replicated, may hold values from 0.1 to 1.9
- routes: int32 [65536, 3], P(('grp', 'ep', 'tp')), parts along dimension 0, may hold values from 0 to 31, all different within a row; in each aligned block of 256 rows (0 to 255, 256 to 511, ...) at most 36 rows name the same one
- gates: float32 [65536, 3], P(('grp', 'ep', 'tp')), parts along dimension 0, may hold values from 0.2 to 1.2
- expert_gate: bfloat16 [32, 2048, 512], P('ep', None, 'tp'), may hold values from -0.125 to 0.125
- expert_up: bfloat16 [32, 2048, 512], P('ep', None, 'tp'), may hold values from -0.125 to 0.125
- expert_down: bfloat16 [32, 512, 2048], P('ep', 'tp'), may hold values from -0.25 to 0.25
- shared_gate: bfloat16 [2048, 512], replicated, may hold values from -0.125 to 0.125
- shared_up: bfloat16 [2048, 512], replicated, may hold values from -0.125 to 0.125
- shared_down: bfloat16 [512, 2048], replicated, may hold values from -0.25 to 0.25
Outputs:
- mixed: bfloat16 [65536, 2048], P(('grp', 'ep', 'tp')), parts along dimension 0
The draws below stay inside these ranges and needn't reach their ends.
There are 4 independent parts, one for each index of `grp`. The reference program is written for one: setup_inputs(seed, part) draws one part's arguments, and reference() takes and returns one part's arrays. A program takes and returns all parts, laid end to end along the dimension named above; an argument that names none is the same for every part. Nothing has to cross between parts.
Inputs may be any that keep to these rules, and one draw needn't show every extreme that they name: `routes`: A row names 3 different experts. Among the rows of one device no expert is named by more than 36 rows, and in every draw some expert is named by exactly 36 rows of some device.
All inputs are finite; a program needn't handle non-finite values.
Results may differ from the reference program's by a relative error of at most 0.01.
Values may be sent and summed in bfloat16 or wider, within the bound.
A program may use at most 128 MiB of HBM per device.

```python
import math
import jax
import jax.numpy as jnp
import numpy as np
from jax import lax

D = 2048
FE = 512
SH_FE = 512
TOP = 3
TOK_DEV = 256
EXPERTS = 32
CAP = 36
TOKENS = 16384
N_EP = 32
N_TP = 2


def level_of(stream_key, extent, pieces, low, top_value):
    factor_of = 1.0
    for dim, parts in pieces:
        draws = jax.random.uniform(jax.random.fold_in(jax.random.fold_in(stream_key, 6), dim), (parts,), jnp.float32, low / len(pieces), top_value / len(pieces))
        factor_of = factor_of * jnp.repeat(jnp.exp(draws), extent[dim] // parts).reshape((-1,) + (1,) * (len(extent) - 1 - dim))
    return factor_of


def routed_block(rng, own, number, rows, number_of, top, limit, skew):
    order = jax.random.permutation(rng, number_of)
    crowded, common = shares(number_of, rows * top, limit, skew, True), shares(number_of, rows * top, limit, skew, False)
    places = jnp.arange(number_of)

    def named(lengths, turn):
        used = int((lengths > 0).sum())
        fixed = max(1, used // 4)
        moved = fixed + (places - fixed + turn * (used - fixed)) % max(1, number_of - fixed)
        return jnp.zeros((number_of,), jnp.int32).at[order[jnp.where(places < fixed, places, moved)]].set(jnp.asarray(lengths, jnp.int32))

    lengths = jnp.where(number % 4 == 0, named(crowded, number // 4), named(common, number - number // 4 - 1))
    mixed = jax.random.permutation(jax.random.fold_in(own, 3), number_of)
    donor, taker = mixed[0:number_of // 2 * 2:2], mixed[1:number_of // 2 * 2:2]
    margin = jnp.minimum(lengths[donor] - 1, limit - lengths[taker]) // 2
    margin = jnp.where((donor == order[0]) | (taker == order[0]) | (lengths[taker] == 0), 0, jnp.maximum(margin, 0))
    moved = jax.random.randint(jax.random.fold_in(own, 4), (number_of // 2,), 0, 1 << 20) % (margin + 1)
    lengths = lengths.at[donor].add(-moved).at[taker].add(moved)
    labels = jnp.searchsorted(jnp.cumsum(lengths), jnp.arange(rows * top), side="right").astype(jnp.int32)
    listing = labels.reshape(top, rows).T
    listing = listing[jax.random.permutation(jax.random.fold_in(own, 1), rows)]
    turn = jax.random.randint(jax.random.fold_in(own, 2), (rows, 1), 0, top)
    return jnp.take_along_axis(listing, (jnp.arange(top)[None, :] + turn) % top, axis=1)


def shares(count, total, limit, skew, full):
    loads = [(1 << 20) // math.isqrt(rank ** skew) + 1 for rank in range(1, count + 1)]
    largest = limit if full else min(limit, max(-(-total // count), total * loads[0] // sum(loads)))
    least = 1 if total - largest >= count - 1 else 0
    given, spare = [largest] + [least] * (count - 1), total - largest - least * (count - 1)
    while spare > 0:
        free = [i for i in range(1, count) if given[i] < largest] or [i for i in range(1, count) if given[i] < limit]
        pool, left = sum([loads[i] for i in free]), spare
        for i in free:
            addition = min(limit - given[i], max(1, left * loads[i] // pool), spare)
            given[i] = given[i] + addition
            spare = spare - addition
    return np.array(given)


def scatter_about(stream_key, dims, deviation, limit, split=(), kind=jnp.bfloat16):
    array = jax.random.normal(stream_key, dims, jnp.float32) * deviation
    if len(split) > 0:
        array = level_of(stream_key, dims, split, -0.22, 0.18) * array
    return jnp.clip(array, min=-limit, max=limit).astype(kind)


def setup_inputs(seed: int = 0, part: int = 0) -> dict:
    splits = jax.random.split(jax.random.key(seed), 11)
    own_keys = jax.random.split(jax.random.fold_in(splits[10], part), 11)
    tokens = scatter_about(own_keys[0], (TOKENS, D), 1.0, 6.0, ((0, 64),))
    norm_gain = jnp.clip(1.0 + 0.18 * jax.random.normal(splits[1], (D,), jnp.float32), 0.1, 1.9)
    routes_keys = jax.random.split(jax.random.fold_in(own_keys[2], 1), TOKENS // TOK_DEV)
    routes_turns = jax.random.permutation(jax.random.fold_in(own_keys[2], 3), TOKENS // TOK_DEV)
    routes = jax.vmap(lambda own, number: routed_block(jax.random.fold_in(own_keys[2], 2), own, number, TOK_DEV, EXPERTS, TOP, CAP, 2))(routes_keys, routes_turns).reshape((TOKENS, TOP))
    gates = jnp.clip(0.2 + 1 * jax.random.uniform(own_keys[3], (TOKENS, TOP), jnp.float32) ** level_of(own_keys[3], (TOKENS, TOP), ((0, 64),), -0.2, 0.2), 0.2, 1.2)
    expert_gate = scatter_about(splits[4], (EXPERTS, D, FE), D ** -0.5, 0.125, ((0, 32), (2, 2)))
    expert_up = scatter_about(splits[5], (EXPERTS, D, FE), D ** -0.5, 0.125, ((0, 32), (2, 2)))
    expert_down = scatter_about(splits[6], (EXPERTS, FE, D), FE ** -0.5, 0.25, ((0, 32), (1, 2)))
    shared_gate = scatter_about(splits[7], (D, SH_FE), D ** -0.5, 0.125)
    shared_up = scatter_about(splits[8], (D, SH_FE), D ** -0.5, 0.125)
    shared_down = scatter_about(splits[9], (SH_FE, D), SH_FE ** -0.5, 0.25)
    return {"tokens": tokens, "norm_gain": norm_gain, "routes": routes, "gates": gates, "expert_gate": expert_gate, "expert_up": expert_up, "expert_down": expert_down, "shared_gate": shared_gate, "shared_up": shared_up, "shared_down": shared_down}


def reference(tokens, norm_gain, routes, gates, expert_gate, expert_up, expert_down, shared_gate, shared_up, shared_down):
    values = tokens.astype(jnp.float32)
    scaling = lax.rsqrt(lax.optimization_barrier(jnp.mean(values * values, axis=1, keepdims=True)) + 1e-06)
    normed = (values * scaling * norm_gain[None, :]).astype(jnp.bfloat16)
    shared_hidden = (jax.nn.silu(jnp.dot(normed, shared_gate, preferred_element_type=jnp.float32)) * jnp.dot(normed, shared_up, preferred_element_type=jnp.float32)).astype(jnp.bfloat16)
    shared_out = jnp.dot(shared_hidden, shared_down, preferred_element_type=jnp.float32)
    token_count = tokens.shape[0]
    top_count = routes.shape[1]
    flat_routes = routes.reshape(-1)
    bound = N_EP * N_TP * CAP
    padded = jnp.concatenate([normed, jnp.zeros((1, D), jnp.bfloat16)], axis=0)
    weights = jnp.concatenate([gates.reshape(-1), jnp.zeros((1,), jnp.float32)], axis=0)

    def one_expert(totals, expert_index):
        picks = jnp.nonzero(flat_routes == expert_index, size=bound, fill_value=token_count * top_count)[0].astype(jnp.int32)
        owners = (picks // top_count).astype(jnp.int32)
        chosen = padded[owners]
        hidden = (jax.nn.silu(jnp.dot(chosen, expert_gate[expert_index], preferred_element_type=jnp.float32)) * jnp.dot(chosen, expert_up[expert_index], preferred_element_type=jnp.float32)).astype(jnp.bfloat16)
        result = jnp.dot(hidden, expert_down[expert_index], preferred_element_type=jnp.float32).astype(jnp.bfloat16)
        weighted = result.astype(jnp.float32) * weights[picks][:, None]
        return (totals.at[owners].add(weighted), None)
    start_totals = jnp.zeros((token_count + 1, D), jnp.float32)
    totals, _ = lax.scan(one_expert, start_totals, jnp.arange(EXPERTS, dtype=jnp.int32))
    return (shared_out + totals[:token_count]).astype(jnp.bfloat16)
```

```python
import functools

import jax
import jax.numpy as jnp
from jax import lax
from jax.experimental import pallas as pl
from jax.experimental.pallas import tpu as pltpu
from jax.sharding import PartitionSpec as P

MESH = pl.DeviceIdType.MESH
BLOCK = 32


def plan(n, rows, cap):
    reach = (n // 2, n - 1 - n // 2)
    carried = []
    for far in reach:
        table = [rows]
        for hop in range(1, far + 1):
            need = cap * (far + 1 - hop)
            table.append(min(rows, -(-need // BLOCK) * BLOCK))
        carried.append(table)
    full = 1
    while all(full + 1 < len(t) and t[full + 1] == rows for t in carried):
        full += 1
    return reach, carried, full


def pieces(count, rows):
    for first in (rows // 2, rows // 4):
        if count > first:
            return ((0, first), (first, count - first))
    return ((0, count),)


def kernel(
    n, rows, cap, top,
    meta_in, rows_in, wg_in, wu_in, wd_in, out,
    x, cs, ct, wg, wu, wd, meta, g,
    in_sem, w_sem, wsend_sem, wrecv_sem,
    msend_sem, mrecv_sem, dsend_sem, drecv_sem, csend_sem, crecv_sem, out_sem,
):
    reach, carried, full = plan(n, rows, cap)
    z, core = lax.axis_index("ep"), lax.axis_index("tp")
    sign = 1 - 2 * core
    up = lax.rem(z + sign + n, n)
    down = lax.rem(z - sign + n, n)
    ahead, back = (up, down), (down, up)
    half = rows // 2
    far = reach[0]
    tail_at = []
    for d in range(2):
        at, table = 0, {}
        for hop in range(reach[d], full, -1):
            table[hop] = at
            at += carried[d][hop]
        tail_at.append(table)

    row_loads = [pltpu.make_async_copy(rows_in.at[d], x.at[d, 0], in_sem.at[d]) for d in range(2)]
    meta_loads = [pltpu.make_async_copy(meta_in.at[d], meta.at[d, 0], in_sem.at[2 + d]) for d in range(2)]
    for c in row_loads + meta_loads:
        c.start()
    w_pairs = ((wg_in, wg), (wu_in, wu), (wd_in, wd))
    w_loads = [pltpu.make_async_copy(a, b.at[0], w_sem.at[i]) for i, (a, b) in enumerate(w_pairs)]
    for c in w_loads:
        c.start()

    barrier = pltpu.get_barrier_semaphore()
    for who in ({"ep": up}, {"ep": down}, {"tp": 1 - core}):
        pl.semaphore_signal(barrier, inc=1, device_id=who, device_id_type=MESH)
    pl.semaphore_wait(barrier, 3)

    def move(d, t, q):
        start, size = q
        part = pl.ds(start, size)
        k = 0 if start == 0 else 1
        return pltpu.make_async_remote_copy(
            src_ref=x.at[d, t - 1, part], dst_ref=x.at[d, t, part],
            send_sem=dsend_sem.at[d, t, k], recv_sem=drecv_sem.at[d, t, k],
            device_id={"ep": ahead[d]}, device_id_type=MESH,
        )

    def move_meta(d, t):
        return pltpu.make_async_remote_copy(
            src_ref=meta.at[d, t - 1], dst_ref=meta.at[d, t],
            send_sem=msend_sem.at[d, t], recv_sem=mrecv_sem.at[d, t],
            device_id={"ep": ahead[d]}, device_id_type=MESH,
        )

    def weigh(d, h):
        m = meta[d, h].T
        me = z.astype(jnp.float32)
        total = jnp.zeros((rows, 1), jnp.float32)
        for k in range(top):
            total += jnp.where(m[:, k : k + 1] == me, m[:, 4 + k : 5 + k], 0.0)
        g[d, h] = total

    def expert(d, h, start, size):
        part = pl.ds(start, size)
        v = x[d, h, part, :]
        acc = None
        for s in range(2):
            a = jnp.dot(v, wg[s], preferred_element_type=jnp.float32)
            b = jnp.dot(v, wu[s], preferred_element_type=jnp.float32)
            hidden = (a * (1.0 / (1.0 + jnp.exp(-a))) * b).astype(jnp.bfloat16)
            y = jnp.dot(hidden, wd[s], preferred_element_type=jnp.float32)
            acc = y if acc is None else acc + y
        x[d, h, part, :] = (acc * g[d, h, part, :]).astype(jnp.bfloat16)

    def expert_tiles(h, lo, hi):
        size = rows // 4
        first = -(-carried[0][h] // size)

        def tile(i, carry):
            d = jnp.where(i < first, 0, 1)
            start = (i - d * first) * size
            expert(d, h, pl.multiple_of(start, size), size)
            return carry

        lax.fori_loop(lo, hi, tile, 0)

    def tile_count(h):
        size = rows // 4
        return sum(-(-carried[d][h] // size) for d in range(2) if h <= reach[d])

    for d in range(2):
        row_loads[d].wait()
        for q in pieces(carried[d][1], rows):
            move(d, 1, q).start()
        meta_loads[d].wait()
        move_meta(d, 1).start()
    w_moves = [
        pltpu.make_async_remote_copy(
            src_ref=a, dst_ref=b.at[1], send_sem=wsend_sem.at[i], recv_sem=wrecv_sem.at[i],
            device_id={"tp": 1 - core}, device_id_type=MESH,
        )
        for i, (a, b) in enumerate(w_pairs)
    ]
    for c in w_moves:
        c.start()
    for d in range(2):
        weigh(d, 0)
    for c in w_loads:
        c.wait()
    for c in w_moves:
        c.wait()

    def full_hop(t, carry):
        for k in range(2):
            q = (k * half, half)
            for d in range(2):
                if k == 0:
                    move_meta(d, t - 1).wait_recv()
                    move_meta(d, t).start()
                move(d, t - 1, q).wait_recv()
                move(d, t, q).start()
            if k == 0:
                for d in range(2):
                    weigh(d, t - 1)
            for d in range(2):
                move(d, t - 1, q).wait_send()

            def both(d, c):
                expert(d, t - 2, k * half, half)
                return c

            lax.fori_loop(0, 2, both, 0)
        return carry

    lax.fori_loop(2, full + 1, full_hop, 0)

    for t in range(full + 1, far + 1):
        h = t - 2
        count = tile_count(h)
        for k in range(2):
            for d in range(2):
                if t - 1 > reach[d]:
                    continue
                if k == 0:
                    move_meta(d, t - 1).wait_recv()
                    if t <= reach[d]:
                        move_meta(d, t).start()
                came = pieces(carried[d][t - 1], rows)
                if k < len(came):
                    move(d, t - 1, came[k]).wait_recv()
                if t <= reach[d]:
                    goes = pieces(carried[d][t], rows)
                    if k < len(goes):
                        move(d, t, goes[k]).start()
            if k == 0:
                for d in range(2):
                    if t - 1 <= reach[d]:
                        weigh(d, t - 1)
                for d in range(2):
                    for q in pieces(carried[d][t - 1], rows) if t - 1 <= reach[d] else ():
                        move(d, t - 1, q).wait_send()
            expert_tiles(h, *((0, count // 2) if k == 0 else (count // 2, count)))

    def landing(d, h):
        if isinstance(h, int) and h > full:
            return lambda start, size: ct.at[d, pl.ds(tail_at[d][h] + start, size)]
        slot = lax.rem(h - 1, 3)
        return lambda start, size: cs.at[d, slot, pl.ds(start, size)]

    def give(d, h, q):
        start, size = q
        k = 0 if start == 0 else 1
        return pltpu.make_async_remote_copy(
            src_ref=x.at[d, h, pl.ds(start, size)], dst_ref=landing(d, h)(start, size),
            send_sem=csend_sem.at[d, h, k], recv_sem=crecv_sem.at[d, h, k],
            device_id={"ep": back[d]}, device_id_type=MESH,
        )

    def add(d, h, q):
        start, size = q
        strip = 16
        at = landing(d, h + 1)(start, size)

        def one(i, carry):
            s = pl.multiple_of(i * strip, strip)
            mine = x[d, h, pl.ds(start + s, strip), :].astype(jnp.float32)
            theirs = at[pl.ds(s, strip), :].astype(jnp.float32)
            x[d, h, pl.ds(start + s, strip), :] = (mine + theirs).astype(jnp.bfloat16)
            return carry

        lax.fori_loop(0, size // strip, one, 0)

    for h in range(far, full - 1, -1):
        if h == far:
            for d in range(2):
                if far <= reach[d]:
                    for q in pieces(carried[d][far], rows):
                        move(d, far, q).wait_recv()
                    move_meta(d, far).wait_recv()
                    weigh(d, far)
            expert_tiles(far, 0, tile_count(far))
        if h == far - 1:
            for d in range(2):
                for q in pieces(carried[d][far], rows) if far <= reach[d] else ():
                    move(d, far, q).wait_send()
            expert_tiles(h, 0, tile_count(h))
        taken = [0, 0]
        for k in range(2):
            for d in range(2):
                if h > reach[d]:
                    continue
                goes = pieces(carried[d][h], rows)
                comes = pieces(carried[d][h + 1], rows) if h + 1 <= reach[d] else ()
                if k >= len(goes):
                    continue
                end = goes[k][0] + goes[k][1]
                while taken[d] < len(comes) and comes[taken[d]][0] < end:
                    q = comes[taken[d]]
                    give(d, h + 1, q).wait_recv()
                    add(d, h, q)
                    taken[d] += 1
                give(d, h, goes[k]).start()

    def full_back(i, carry):
        h = full - 1 - i
        for k in range(2):
            q = (k * half, half)
            for d in range(2):
                give(d, h + 1, q).wait_recv()
                add(d, h, q)
                give(d, h, q).start()
        return carry

    lax.fori_loop(0, full - 1, full_back, 0)

    results = []
    for k in range(2):
        q = (k * half, half)
        for d in range(2):
            give(d, 1, q).wait_recv()
            add(d, 0, q)
            part = pl.ds(k * half, half)
            results.append(pltpu.make_async_copy(x.at[d, 0, part], out.at[d, part], out_sem.at[d, k]))
            results[-1].start()

    for d in range(2):
        for h in range(full, reach[d] + 1):
            for q in pieces(carried[d][h], rows):
                give(d, h, q).wait_send()

    def drain(h, carry):
        for d in range(2):
            for k in range(2):
                give(d, h, (k * half, half)).wait_send()
        return carry

    lax.fori_loop(1, full, drain, 0)

    def drain_meta(t, carry):
        for d in range(2):
            move_meta(d, t).wait_send()
        return carry

    lax.fori_loop(1, reach[1] + 1, drain_meta, 0)
    for t in range(reach[1] + 1, far + 1):
        move_meta(0, t).wait_send()
    for c in results:
        c.wait()


def exchange(n, cap, meta, sent, w_gate, w_up, w_down):
    _, rows, width = sent.shape
    top = 3
    hidden = w_gate.shape[1]
    reach, carried, full = plan(n, rows, cap)
    slots = reach[0] + 1
    tail = max(sum(carried[d][full + 1 :]) for d in range(2))
    any_space = pl.BlockSpec(memory_space=pl.ANY)
    dma = pltpu.SemaphoreType.DMA
    return pl.pallas_call(
        functools.partial(kernel, n, rows, cap, top),
        out_shape=jax.ShapeDtypeStruct((2, rows, width), jnp.bfloat16),
        in_specs=[any_space] * 5,
        out_specs=any_space,
        scratch_shapes=[
            pltpu.VMEM((2, slots, rows, width), jnp.bfloat16),
            pltpu.VMEM((2, 3, rows, width), jnp.bfloat16),
            pltpu.VMEM((2, tail, width), jnp.bfloat16),
            pltpu.VMEM((2, width, hidden), jnp.bfloat16),
            pltpu.VMEM((2, width, hidden), jnp.bfloat16),
            pltpu.VMEM((2, hidden, width), jnp.bfloat16),
            pltpu.VMEM((2, slots, 8, rows), jnp.float32),
            pltpu.VMEM((2, slots, rows, 1), jnp.float32),
            dma((4,)),
            dma((3,)),
            dma((3,)),
            dma((3,)),
            dma((2, slots)),
            dma((2, slots)),
            dma((2, slots, 2)),
            dma((2, slots, 2)),
            dma((2, slots, 2)),
            dma((2, slots, 2)),
            dma((2, 2)),
        ],
        compiler_params=pltpu.CompilerParams(
            collective_id=0, has_side_effects=True, vmem_limit_bytes=67043328
        ),
        name="exchange",
    )(meta, sent, w_gate, w_up, w_down)


def on_device(
    tokens,
    norm_gain,
    routes,
    gates,
    expert_gate,
    expert_up,
    expert_down,
    shared_gate,
    shared_up,
    shared_down,
):
    rows, width = tokens.shape
    top = routes.shape[1]
    n = lax.axis_size("ep")
    cap = 3 * rows * top // (2 * n)
    z, core = lax.axis_index("ep"), lax.axis_index("tp")
    values = tokens.astype(jnp.float32)
    scaling = lax.rsqrt(jnp.mean(values * values, axis=1, keepdims=True) + 1e-06)
    normed = (values * scaling * norm_gain[None, :]).astype(jnp.bfloat16)

    forward = jnp.mod((routes - z) * (1 - 2 * core), n)
    first = forward <= n // 2
    distance = jnp.stack([jnp.where(first, forward, 0), jnp.where(first, 0, n - forward)])
    farthest = jnp.max(distance, axis=2)
    own = farthest[:, :, None]
    other = farthest[:, None, :]
    index = jnp.arange(rows, dtype=jnp.int32)
    before = (other > own) | ((other == own) & (index[None, None, :] < index[None, :, None]))
    rank = jnp.sum(before.astype(jnp.int32), axis=2)
    chosen = rank[:, None, :] == index[None, :, None]
    order = chosen.astype(jnp.bfloat16)
    sent = jnp.einsum("drt,tw->drw", order, normed, preferred_element_type=jnp.float32)
    sent = sent.astype(jnp.bfloat16)
    names = jnp.where(jnp.stack([first, ~first]), routes[None], -1).astype(jnp.float32)
    blank = jnp.zeros((2, rows, 4 - top), jnp.float32)
    facts = jnp.concatenate(
        [names, blank, jnp.broadcast_to(gates[None], names.shape), blank], axis=2
    )
    meta = jnp.sum(
        jnp.where(chosen[:, None, :, :], jnp.swapaxes(facts, 1, 2)[:, :, None, :], 0.0), axis=3
    )

    parts = exchange(n, cap, meta, sent, expert_gate[0], expert_up[0], expert_down[0])

    shared_hidden = (
        jax.nn.silu(jnp.dot(normed, shared_gate, preferred_element_type=jnp.float32))
        * jnp.dot(normed, shared_up, preferred_element_type=jnp.float32)
    ).astype(jnp.bfloat16)
    shared_out = jnp.dot(shared_hidden, shared_down, preferred_element_type=jnp.float32)
    routed = jnp.einsum("drt,drw->tw", order, parts, preferred_element_type=jnp.float32)
    return (shared_out + routed).astype(jnp.bfloat16)


def solution(mesh):
    return jax.shard_map(
        on_device,
        mesh=mesh,
        in_specs=(
            P(("grp", "ep", "tp"), None),
            P(),
            P(("grp", "ep", "tp"), None),
            P(("grp", "ep", "tp"), None),
            P("ep", None, "tp"),
            P("ep", None, "tp"),
            P("ep", "tp", None),
            P(),
            P(),
            P(),
        ),
        out_specs=P(("grp", "ep", "tp"), None),
        check_vma=False,
    )
```
